32 devices in a mesh: sp: 8 (over z, x), tp: 4 (over y, core).
Axes of the slice: x: 2, y: 2, z: 4, core: 2. Of those that a mesh axis runs over, the one named last changes fastest.
Arguments:
- queries: bfloat16 [2560, 1024], P('sp', 'tp'), may hold values from -6.6 to 6.6
- key_matrix: bfloat16 [2560, 256], P('sp', 'tp'), may hold values from -6.6 to 6.6
- values: bfloat16 [2560, 256], P('sp', 'tp'), may hold values from -6 to 6
- query_gain: float32 [64], replicated, may hold values from 0.19 to 8
- key_norm_gain: float32 [64], replicated, may hold values from 0.19 to 8
- head_gain: float32 [1024], P('tp'), may hold values from 0.1 to 1.9
- out_proj: bfloat16 [1024, 2048], replicated, may hold values from -0.1875 to 0.1875
- residual: bfloat16 [2560, 2048], P('sp'), may hold values from -6 to 6
- ffn_gain: float32 [2048], replicated, may hold values from 0.1 to 1.9
- routes: int32 [2560, 4], P('sp'), may hold values from 0 to 31, all different within a row; in each aligned block of 320 rows (0 to 319, 320 to 639, ...) at most 80 rows name the same one
- route_weights: float32 [2560, 4], P('sp'), may hold values from 0.2 to 1
- expert_gate: bfloat16 [32, 2048, 512], P(('sp', 'tp')), may hold values from -0.125 to 0.125
- expert_up: bfloat16 [32, 2048, 512], P(('sp', 'tp')), may hold values from -0.125 to 0.125
- expert_down: bfloat16 [32, 512, 2048], P(('sp', 'tp')), may hold values from -0.25 to 0.25
- shared_gate: bfloat16 [2048, 512], P(None, 'tp'), may hold values from -0.125 to 0.125
- shared_up: bfloat16 [2048, 512], P(None, 'tp'), may hold values from -0.125 to 0.125
- shared_down: bfloat16 [512, 2048], P('tp'), may hold values from -0.25 to 0.25
Outputs:
- layer_out: bfloat16 [2560, 2048], P(('sp', 'tp'))
The draws below stay inside these ranges and needn't reach their ends.
Inputs may be any that keep to these rules, and one draw needn't show every extreme that they name: `routes`: each row names 4 different experts; in each aligned block of 320 rows (the tokens of one index of sp) no expert is named more than 80 times, a bound that some block reaches.
All inputs are finite; a program needn't handle non-finite values.
Results may differ from the reference program's by a relative error of at most 0.019.
The reference program's roundings to bfloat16 on the way count: a program that leaves them out, or rounds other values in their place, can miss the bound.
Values may be sent and summed in bfloat16 or wider, within the bound.
No kernel may reach another device: no remote copies, remote signals or barrier semaphores. Data moves between devices by JAX's collectives and lax.ppermute only.
A program may use at most 128 MiB of HBM per device.

```python
import math
import jax
import jax.numpy as jnp
import numpy as np
from jax import lax

D = 2048
HEAD_SIZE = 64
QUERY_HEADS = 16
KEY_VALUE_HEADS = 4
FF = 512
SFF = 512
TOPK = 4
GRID_W = 64
TOK_DEV = 320
SEQUENCE_TOKENS = 2560
EXPERTS = 32
CAP = 80
N_SP = 8
N_TP = 4


def plant_pair(key):
    unrotated_query = jnp.clip(jax.random.normal(jax.random.fold_in(key, 11), (SEQUENCE_TOKENS, QUERY_HEADS * HEAD_SIZE), jnp.float32), -6.0, 6.0)
    unrotated_key = jnp.clip(jax.random.normal(jax.random.fold_in(key, 12), (SEQUENCE_TOKENS, KEY_VALUE_HEADS * HEAD_SIZE), jnp.float32), -6.0, 6.0)
    return (unrotated_query, unrotated_key)


def draw_queries(key, part):
    return plant_pair(key)[0].astype(jnp.bfloat16)


def draw_key_matrix(key, part):
    return plant_pair(key)[1].astype(jnp.bfloat16)


def gain_draw(key, salt):
    folded = jax.random.fold_in(key, salt)
    return 1.0 + 0.18 * jnp.clip(jax.random.normal(folded, (HEAD_SIZE,), jnp.float32), -4.5, 4.5)


def draw_query_gain(key, part):
    return gain_draw(key, 21)


def draw_key_norm_gain(key, part):
    return gain_draw(key, 22)


def block_scale(key, dims, cuts, smallest, top_value):
    factor_of, own = 1.0, jax.random.fold_in(key, 6)
    for axis_at, parts in cuts:
        heights = jnp.exp(jax.random.uniform(jax.random.fold_in(own, axis_at), (parts,), jnp.float32, smallest / len(cuts), top_value / len(cuts)))
        factor_of = factor_of * jnp.repeat(heights, dims[axis_at] // parts).reshape([-1 if axis == axis_at else 1 for axis in range(len(dims))])
    return factor_of


def routed_block(own_key, own, number, rows, amount, top, limit, skew):
    order = jax.random.permutation(own_key, amount)
    packed, common = portions_of(amount, rows * top, limit, skew, True), portions_of(amount, rows * top, limit, skew, False)
    places = jnp.arange(amount)

    def named(tallies, rotation):
        used = int((tallies > 0).sum())
        fixed = max(1, used // 4)
        passed = fixed + (places - fixed + rotation * (used - fixed)) % max(1, amount - fixed)
        return jnp.zeros((amount,), jnp.int32).at[order[jnp.where(places < fixed, places, passed)]].set(jnp.asarray(tallies, jnp.int32))

    tallies = jnp.where(number % 4 == 0, named(packed, number // 4), named(common, number - number // 4 - 1))
    mixed = jax.random.permutation(jax.random.fold_in(own, 3), amount)
    source_of, receiver = mixed[0:amount // 2 * 2:2], mixed[1:amount // 2 * 2:2]
    room = jnp.minimum(tallies[source_of] - 1, limit - tallies[receiver]) // 2
    room = jnp.where((source_of == order[0]) | (receiver == order[0]) | (tallies[receiver] == 0), 0, jnp.maximum(room, 0))
    passed = jax.random.randint(jax.random.fold_in(own, 4), (amount // 2,), 0, 1 << 20) % (room + 1)
    tallies = tallies.at[source_of].add(-passed).at[receiver].add(passed)
    items = jnp.searchsorted(jnp.cumsum(tallies), jnp.arange(rows * top), side="right").astype(jnp.int32)
    grid = items.reshape(top, rows).T
    grid = grid[jax.random.permutation(jax.random.fold_in(own, 1), rows)]
    rotation = jax.random.randint(jax.random.fold_in(own, 2), (rows, 1), 0, top)
    return jnp.take_along_axis(grid, (jnp.arange(top)[None, :] + rotation) % top, axis=1)


def portions_of(number_of, total, limit, slope, full):
    weights = [(1 << 20) // math.isqrt(rank ** slope) + 1 for rank in range(1, number_of + 1)]
    largest = limit if full else min(limit, max(-(-total // number_of), total * weights[0] // sum(weights)))
    least = 1 if total - largest >= number_of - 1 else 0
    given, surplus = [largest] + [least] * (number_of - 1), total - largest - least * (number_of - 1)
    while surplus > 0:
        free = [i for i in range(1, number_of) if given[i] < largest] or [i for i in range(1, number_of) if given[i] < limit]
        whole, left = sum([weights[i] for i in free]), surplus
        for i in free:
            addition = min(limit - given[i], max(1, left * weights[i] // whole), surplus)
            given[i] = given[i] + addition
            surplus = surplus - addition
    return np.array(given)


def normal_values(rng, dims, spread, reach, cuts=(), kind=jnp.bfloat16):
    values = spread * jax.random.normal(rng, dims, jnp.float32)
    if cuts:
        values = values * block_scale(rng, dims, cuts, -0.22, 0.18)
    return jnp.clip(values, -reach, reach).astype(kind)


def setup_inputs(seed: int = 0) -> dict:
    seeds = jax.random.split(jax.random.key(seed), 18)
    queries = draw_queries(jax.random.fold_in(seeds[17], 71), 0)
    key_matrix = draw_key_matrix(jax.random.fold_in(seeds[17], 71), 0)
    values = normal_values(seeds[2], (SEQUENCE_TOKENS, KEY_VALUE_HEADS * HEAD_SIZE), 1.0, 6.0, ((0, 8), (1, 4)))
    query_gain = draw_query_gain(jax.random.fold_in(seeds[17], 71), 0)
    key_norm_gain = draw_key_norm_gain(jax.random.fold_in(seeds[17], 71), 0)
    head_gain = jnp.clip(1.0 + 0.18 * jax.random.normal(seeds[5], (QUERY_HEADS * HEAD_SIZE,), jnp.float32), 0.1, 1.9)
    out_proj = normal_values(seeds[6], (QUERY_HEADS * HEAD_SIZE, D), (QUERY_HEADS * HEAD_SIZE) ** -0.5, 0.1875)
    residual = normal_values(seeds[7], (SEQUENCE_TOKENS, D), 1.0, 6.0, ((0, 8),))
    ffn_gain = jnp.clip(1.0 + 0.18 * jax.random.normal(seeds[8], (D,), jnp.float32), 0.1, 1.9)
    routes_keys = jax.random.split(jax.random.fold_in(seeds[9], 1), SEQUENCE_TOKENS // TOK_DEV)
    routes_turns = jax.random.permutation(jax.random.fold_in(seeds[9], 3), SEQUENCE_TOKENS // TOK_DEV)
    routes = jax.vmap(lambda own, number: routed_block(jax.random.fold_in(seeds[9], 2), own, number, TOK_DEV, EXPERTS, TOPK, CAP, 1))(routes_keys, routes_turns).reshape((SEQUENCE_TOKENS, TOPK))
    route_weights = jnp.clip(0.2 + 0.8 * jax.random.uniform(seeds[10], (SEQUENCE_TOKENS, TOPK), jnp.float32) ** block_scale(seeds[10], (SEQUENCE_TOKENS, TOPK), ((0, 8),), -0.2, 0.2), 0.2, 1.0)
    expert_gate = normal_values(seeds[11], (EXPERTS, D, FF), D ** -0.5, 0.125, ((0, 32),))
    expert_up = normal_values(seeds[12], (EXPERTS, D, FF), D ** -0.5, 0.125, ((0, 32),))
    expert_down = normal_values(seeds[13], (EXPERTS, FF, D), FF ** -0.5, 0.25, ((0, 32),))
    shared_gate = normal_values(seeds[14], (D, SFF), D ** -0.5, 0.125, ((1, 4),))
    shared_up = normal_values(seeds[15], (D, SFF), D ** -0.5, 0.125, ((1, 4),))
    shared_down = normal_values(seeds[16], (SFF, D), SFF ** -0.5, 0.25, ((0, 4),))
    return dict(queries=queries, key_matrix=key_matrix, values=values, query_gain=query_gain, key_norm_gain=key_norm_gain, head_gain=head_gain, out_proj=out_proj, residual=residual, ffn_gain=ffn_gain, routes=routes, route_weights=route_weights, expert_gate=expert_gate, expert_up=expert_up, expert_down=expert_down, shared_gate=shared_gate, shared_up=shared_up, shared_down=shared_down)


EPS = 1e-06
THETA = 10000.0

def final_norm(field, gain):
    mean_sq = lax.optimization_barrier(jnp.mean(field * field, axis=-1, keepdims=True))
    return field * lax.rsqrt(mean_sq + EPS) * gain

def grid_tables(positions, sequence_total):
    grid_rows = sequence_total // GRID_W
    row_pos = (positions // GRID_W - grid_rows // 2).astype(jnp.float32)
    col_pos = (positions % GRID_W - GRID_W // 2).astype(jnp.float32)
    quarter = HEAD_SIZE // 4
    inverse = THETA ** (-jnp.arange(quarter, dtype=jnp.float32) / quarter)
    angles = jnp.concatenate([row_pos[:, None] * inverse, col_pos[:, None] * inverse], axis=1)
    return (jnp.cos(angles), jnp.sin(angles))

def apply_rotary(field, cosine_table, sine_table):
    row_count, head_count = (field.shape[0], field.shape[1])
    quarter = HEAD_SIZE // 4
    pieces = field.reshape(row_count, head_count, 2, 2, quarter)
    front_half = pieces[:, :, :, 0, :].reshape(row_count, head_count, 2 * quarter)
    back_half = pieces[:, :, :, 1, :].reshape(row_count, head_count, 2 * quarter)
    cos_wide = cosine_table[:, None, :]
    sin_wide = sine_table[:, None, :]
    new_front = (front_half * cos_wide - back_half * sin_wide).reshape(row_count, head_count, 2, 1, quarter)
    new_back = (front_half * sin_wide + back_half * cos_wide).reshape(row_count, head_count, 2, 1, quarter)
    return jnp.concatenate([new_front, new_back], axis=3).reshape(row_count, head_count, HEAD_SIZE)

def reference(queries, key_matrix, values, query_gain, key_norm_gain, head_gain, out_proj, residual, ffn_gain, routes, route_weights, expert_gate, expert_up, expert_down, shared_gate, shared_up, shared_down):
    sequence_total = SEQUENCE_TOKENS
    positions = jnp.arange(sequence_total, dtype=jnp.int32)
    cosine_table, sine_table = grid_tables(positions, sequence_total)
    rotated_query = apply_rotary(final_norm(queries.astype(jnp.float32).reshape(sequence_total, QUERY_HEADS, HEAD_SIZE), query_gain), cosine_table, sine_table).astype(jnp.bfloat16)
    rotated_key = apply_rotary(final_norm(key_matrix.astype(jnp.float32).reshape(sequence_total, KEY_VALUE_HEADS, HEAD_SIZE), key_norm_gain), cosine_table, sine_table).astype(jnp.bfloat16)
    group_width = QUERY_HEADS // KEY_VALUE_HEADS
    block_length = 64
    query_block_list = rotated_query.reshape(sequence_total // block_length, block_length, KEY_VALUE_HEADS, group_width, HEAD_SIZE)
    key_wide = rotated_key.astype(jnp.float32)
    value_expanded = values.reshape(sequence_total, KEY_VALUE_HEADS, HEAD_SIZE).astype(jnp.float32)
    score_scale = HEAD_SIZE ** (-0.5)

    def attend(query_block):
        scores = jnp.einsum('qkgd,skd->kgqs', query_block.astype(jnp.float32), key_wide) * score_scale
        row_max = lax.optimization_barrier(jnp.max(scores, axis=-1, keepdims=True))
        expo_terms = jnp.exp(scores - row_max)
        weights = lax.optimization_barrier(expo_terms.astype(jnp.bfloat16)).astype(jnp.float32)
        mixed_vals = jnp.einsum('kgqs,skd->qkgd', weights, value_expanded)
        denominator = jnp.moveaxis(lax.optimization_barrier(jnp.sum(expo_terms, axis=-1)), -1, 0)
        return mixed_vals / denominator[..., None]
    attended = lax.map(attend, query_block_list).reshape(sequence_total, QUERY_HEADS, HEAD_SIZE)
    head_out = final_norm(attended, head_gain.reshape(QUERY_HEADS, HEAD_SIZE)).astype(jnp.bfloat16).reshape(sequence_total, QUERY_HEADS * HEAD_SIZE)
    hidden = (residual.astype(jnp.float32) + jnp.dot(head_out, out_proj, preferred_element_type=jnp.float32)).astype(jnp.bfloat16)
    normed = final_norm(hidden.astype(jnp.float32), ffn_gain).astype(jnp.bfloat16)
    flat_expert = routes.reshape(-1).astype(jnp.int32)
    entries = flat_expert.shape[0]
    order_ids = jnp.argsort(flat_expert, stable=True).astype(jnp.int32)
    sorted_expert = flat_expert[order_ids]
    counts_per = jnp.bincount(flat_expert, length=EXPERTS).astype(jnp.int32)
    starts = (jnp.cumsum(counts_per) - counts_per).astype(jnp.int32)
    rank_ids = (jnp.arange(entries, dtype=jnp.int32) - starts[sorted_expert]).astype(jnp.int32)
    slot_table = jnp.full((EXPERTS, N_SP * CAP), entries, jnp.int32).at[sorted_expert, rank_ids].set(order_ids)
    entry_weight = jnp.concatenate([route_weights.reshape(-1), jnp.zeros((1,), jnp.float32)])
    entry_token = jnp.concatenate([jnp.arange(entries, dtype=jnp.int32) // TOPK, jnp.zeros((1,), jnp.int32)])
    slice_width = SFF // N_TP
    result = hidden.astype(jnp.float32)
    for owner in range(N_TP):
        col_start = owner * slice_width
        gate_part = jnp.dot(normed, shared_gate[:, col_start:col_start + slice_width], preferred_element_type=jnp.float32)
        up_part = jnp.dot(normed, shared_up[:, col_start:col_start + slice_width], preferred_element_type=jnp.float32)
        inner_act = (jax.nn.silu(gate_part) * up_part).astype(jnp.bfloat16)
        partial_sum = jnp.dot(inner_act, shared_down[col_start:col_start + slice_width, :], preferred_element_type=jnp.float32)

        def add_expert(total_acc, local_index, owner=owner):
            expert = local_index * N_TP + owner
            entry_ids = slot_table[expert]
            token_ids = entry_token[entry_ids]
            rows_in = normed[token_ids]
            gate_out = jnp.dot(rows_in, expert_gate[expert], preferred_element_type=jnp.float32)
            up_out = jnp.dot(rows_in, expert_up[expert], preferred_element_type=jnp.float32)
            expert_inner = (jax.nn.silu(gate_out) * up_out).astype(jnp.bfloat16)
            produced = jnp.dot(expert_inner, expert_down[expert], preferred_element_type=jnp.float32).astype(jnp.bfloat16)
            weighted = produced.astype(jnp.float32) * entry_weight[entry_ids][:, None]
            return (total_acc.at[token_ids].add(weighted), None)
        partial_sum, _ = lax.scan(add_expert, partial_sum, jnp.arange(EXPERTS // N_TP, dtype=jnp.int32))
        result = result + lax.optimization_barrier(partial_sum.astype(jnp.bfloat16)).astype(jnp.float32)
    return result.astype(jnp.bfloat16)
```

```python
import jax
import jax.numpy as jnp
from jax import lax
from jax.sharding import PartitionSpec as P

HEAD_SIZE = 64
GRID_W = 64


EPS = 1e-06
THETA = 10000.0


def final_norm(field, gain):
    mean_sq = jnp.mean(field * field, axis=-1, keepdims=True)
    return field * lax.rsqrt(mean_sq + EPS) * gain


def grid_tables(positions, sequence_total):
    grid_rows = sequence_total // GRID_W
    row_pos = (positions // GRID_W - grid_rows // 2).astype(jnp.float32)
    col_pos = (positions % GRID_W - GRID_W // 2).astype(jnp.float32)
    quarter = HEAD_SIZE // 4
    inverse = THETA ** (-jnp.arange(quarter, dtype=jnp.float32) / quarter)
    angles = jnp.concatenate([row_pos[:, None] * inverse, col_pos[:, None] * inverse], axis=1)
    return (jnp.cos(angles), jnp.sin(angles))


def apply_rotary(field, cosine_table, sine_table):
    row_count, head_count = (field.shape[0], field.shape[1])
    quarter = HEAD_SIZE // 4
    pieces = field.reshape(row_count, head_count, 2, 2, quarter)
    front_half = pieces[:, :, :, 0, :].reshape(row_count, head_count, 2 * quarter)
    back_half = pieces[:, :, :, 1, :].reshape(row_count, head_count, 2 * quarter)
    cos_wide = cosine_table[:, None, :]
    sin_wide = sine_table[:, None, :]
    new_front = (front_half * cos_wide - back_half * sin_wide).reshape(
        row_count, head_count, 2, 1, quarter
    )
    new_back = (front_half * sin_wide + back_half * cos_wide).reshape(
        row_count, head_count, 2, 1, quarter
    )
    return jnp.concatenate([new_front, new_back], axis=3).reshape(row_count, head_count, HEAD_SIZE)


def key_block_rows(piece_rows):
    return max((width for width in range(1, 2049) if piece_rows % width == 0))


def swap(field, axis, offset):
    size = lax.axis_size(axis)
    return lax.ppermute(field, axis, [(s, s ^ offset) for s in range(size)])


def by_offset(field, tp_index, tp_count):
    rows = field.shape[0] // tp_count
    return jnp.concatenate(
        [
            lax.dynamic_slice_in_dim(field, jnp.bitwise_xor(tp_index, o) * rows, rows, 0)
            for o in range(tp_count)
        ],
        axis=0,
    )


def gather_offsets(field, tp_count):
    held = {0: field}
    bit = tp_count // 2
    while bit:
        keys = sorted(held)
        sent = jnp.concatenate([held[k] for k in keys], axis=0)
        got = swap(sent, "tp", bit)
        for n, piece in enumerate(jnp.split(got, len(keys), axis=0)):
            held[keys[n] | bit] = piece
        bit //= 2
    return jnp.concatenate([held[k] for k in range(tp_count)], axis=0)


def scatter_offsets(field, tp_count):
    rows = field.shape[0] // tp_count
    pieces = [field[o * rows : (o + 1) * rows] for o in range(tp_count)]
    bit = 1
    while len(pieces) > 1:
        sent = jnp.concatenate([p.astype(jnp.bfloat16) for p in pieces[1::2]], axis=0)
        got = jnp.split(swap(sent, "tp", bit), len(pieces) // 2, axis=0)
        pieces = [p + g.astype(jnp.float32) for p, g in zip(pieces[0::2], got)]
        bit *= 2
    return pieces[0]


def by_block(sp_index, tp_index):
    half = lax.axis_size("sp") // 2
    offsets = jnp.arange(half, dtype=jnp.int32)
    first = (sp_index // half) * half
    targets = first + offsets if half > 8 else jnp.bitwise_xor(sp_index, offsets)
    return targets * lax.axis_size("tp") + tp_index


def slot_map(table, names, sp_index, tp_index):
    topk_count = table.shape[0] // 2
    tokens = table.shape[1]
    experts = names(sp_index, tp_index).astype(jnp.float32)
    match = jnp.zeros((experts.shape[0], tokens), jnp.float32)
    weight = match
    for k in range(topk_count):
        hit = table[k][None, :] == experts[:, None]
        match = match + jnp.where(hit, 1.0, 0.0)
        weight = weight + jnp.where(hit, table[topk_count + k][None, :], 0.0)
    before = jnp.arange(tokens)[:, None] < jnp.arange(tokens)[None, :]
    rank = jnp.dot(
        match.astype(jnp.bfloat16),
        before.astype(jnp.bfloat16),
        preferred_element_type=jnp.float32,
    )
    return match, rank, weight


def filled_slots(match, rank, capacity):
    slots = jnp.arange(capacity, dtype=jnp.int32).astype(jnp.float32)[None, :, None]
    return (rank[:, None, :] == slots) & (match[:, None, :] > 0.5)


def placing(match, rank, capacity):
    filled = filled_slots(match, rank, capacity)
    return jnp.where(filled, 1.0, 0.0).astype(jnp.bfloat16).reshape(-1, match.shape[1])


def weighing(match, rank, weight, capacity):
    filled = filled_slots(match, rank, capacity)
    high = lax.reduce_precision(weight, 8, 7)
    parts = []
    for part in (high, weight - high):
        spread = jnp.where(filled, part[:, None, :], 0.0).astype(jnp.bfloat16)
        parts.append(spread.reshape(-1, match.shape[1]))
    return parts


def collect(back, rows):
    high, low = [
        lax.dot_general(part, rows, (((0,), (0,)), ((), ())), preferred_element_type=jnp.float32)
        for part in back
    ]
    return high + low


def exchange(rows, half, capacity):
    if half > 8:
        size = 2 * half
        groups = [list(range(half)), list(range(half, size))]
        return lax.all_to_all(
            rows.reshape(half, capacity, -1),
            "sp",
            split_axis=0,
            concat_axis=0,
            axis_index_groups=groups,
            tiled=True,
        ).reshape(rows.shape)
    order = sorted(range(half), key=lambda o: -bin(o).count("1"))
    got = {}
    for o in order:
        piece = rows[o * capacity : (o + 1) * capacity]
        got[o] = piece if o == 0 else swap(piece, "sp", o)
    return jnp.concatenate([got[o] for o in range(half)], axis=0)


def gather_blocks(packed, sp_count):
    if sp_count > 8:
        return lax.all_gather(packed, "sp", axis=0, tiled=True)
    order = sorted(range(1, sp_count), reverse=True)
    return jnp.concatenate([swap(packed, "sp", o) for o in order] + [packed], axis=0)


def attention(query_rows, key_values):
    piece_rows = key_values.shape[0]
    block_length = key_block_rows(piece_rows)
    key_blocks = key_values.reshape(piece_rows // block_length, block_length, 2 * HEAD_SIZE)
    score_scale = HEAD_SIZE ** (-0.5)
    rows = query_rows.shape[0]

    def step(carry, key_slab):
        run_max, run_total, run_acc = carry
        scores = (
            lax.dot_general(
                query_rows,
                key_slab[:, :HEAD_SIZE],
                (((1,), (1,)), ((), ())),
                preferred_element_type=jnp.float32,
            )
            * score_scale
        )
        new_max = jnp.maximum(run_max, jnp.max(scores, axis=1))
        factor = jnp.exp(run_max - new_max)
        expo_terms = jnp.exp(scores - new_max[:, None])
        new_total = run_total * factor + jnp.sum(expo_terms, axis=1)
        new_acc = run_acc * factor[:, None] + jnp.dot(
            expo_terms.astype(jnp.bfloat16),
            key_slab[:, HEAD_SIZE:],
            preferred_element_type=jnp.float32,
        )
        return ((new_max, new_total, new_acc), None)

    start = (
        jnp.full((rows,), -1e30, jnp.float32),
        jnp.zeros((rows,), jnp.float32),
        jnp.zeros((rows, HEAD_SIZE), jnp.float32),
    )
    (_, run_total, run_acc), _ = lax.scan(step, start, key_blocks)
    return run_acc / run_total[:, None]


def local(
    queries,
    key_matrix,
    values,
    query_gain,
    key_norm_gain,
    head_gain,
    out_proj,
    residual,
    ffn_gain,
    routes,
    route_weights,
    expert_gate,
    expert_up,
    expert_down,
    shared_gate,
    shared_up,
    shared_down,
):
    tok_count = queries.shape[0]
    head_count = queries.shape[1] // HEAD_SIZE
    sp_count = lax.axis_size("sp")
    tp_count = lax.axis_size("tp")
    tp_index = lax.axis_index("tp")
    sequence_total = tok_count * sp_count
    positions = lax.axis_index("sp") * tok_count + jnp.arange(tok_count, dtype=jnp.int32)
    cosine_table, sine_table = grid_tables(positions, sequence_total)
    rotated_query = apply_rotary(
        final_norm(
            queries.astype(jnp.float32).reshape(tok_count, head_count, HEAD_SIZE), query_gain
        ),
        cosine_table,
        sine_table,
    ).astype(jnp.bfloat16)
    rotated_key = (
        apply_rotary(
            final_norm(
                key_matrix.astype(jnp.float32).reshape(tok_count, 1, HEAD_SIZE), key_norm_gain
            ),
            cosine_table,
            sine_table,
        )
        .reshape(tok_count, HEAD_SIZE)
        .astype(jnp.bfloat16)
    )
    packed = jnp.concatenate([rotated_key, values], axis=1)
    half = sp_count // 2
    sp_index = lax.axis_index("sp")
    part_rows = tok_count // tp_count
    topk_count = routes.shape[1]
    capacity = max(2, 2 * tok_count * topk_count // (sp_count * tp_count))
    table = jnp.concatenate([routes.astype(jnp.float32), route_weights], axis=1)
    own_table = table.T
    mirror_table = by_offset(swap(table, "sp", half), tp_index, tp_count).T
    own_match, own_rank, own_weight = slot_map(own_table, by_block, sp_index, tp_index)
    mir_match, mir_rank, mir_weight = slot_map(mirror_table, by_block, sp_index, tp_index)
    own_send = placing(own_match, own_rank, capacity)
    mir_send = placing(mir_match, mir_rank, capacity)
    own_back = weighing(
        *[by_offset(m.T, tp_index, tp_count).T for m in (own_match, own_rank, own_weight)],
        capacity,
    )
    mir_back = weighing(mir_match, mir_rank, mir_weight, capacity)

    query_rows = rotated_query.transpose(1, 0, 2).reshape(head_count * tok_count, HEAD_SIZE)
    gathered = gather_blocks(packed, sp_count)
    attended = attention(query_rows, gathered).reshape(head_count, tok_count, HEAD_SIZE)
    attended = attended.transpose(1, 0, 2)
    head_out = final_norm(attended, head_gain.reshape(head_count, HEAD_SIZE)).astype(jnp.bfloat16)
    head_out = head_out.reshape(tok_count, head_count * HEAD_SIZE)
    token_heads = lax.all_gather(head_out, "tp", axis=1, tiled=True)
    hidden = (
        residual.astype(jnp.float32)
        + jnp.dot(token_heads, out_proj, preferred_element_type=jnp.float32)
    ).astype(jnp.bfloat16)
    normed = final_norm(hidden.astype(jnp.float32), ffn_gain).astype(jnp.bfloat16)
    model_width = normed.shape[1]
    normed_own = lax.dynamic_slice_in_dim(normed, tp_index * part_rows, part_rows, 0)
    hidden_own = lax.dynamic_slice_in_dim(hidden, tp_index * part_rows, part_rows, 0)

    mirror_rows = gather_offsets(swap(normed_own, "sp", half), tp_count)
    own_out = jnp.dot(own_send, normed, preferred_element_type=jnp.float32).astype(jnp.bfloat16)
    own_arrived = exchange(own_out, half, capacity)
    gate_part = jnp.dot(normed, shared_gate, preferred_element_type=jnp.float32)
    up_part = jnp.dot(normed, shared_up, preferred_element_type=jnp.float32)
    shared_inner = (jax.nn.silu(gate_part) * up_part).astype(jnp.bfloat16)
    shared_inner = by_offset(shared_inner, tp_index, tp_count)
    shared_part = jnp.dot(shared_inner, shared_down, preferred_element_type=jnp.float32)

    mir_out = jnp.dot(mir_send, mirror_rows, preferred_element_type=jnp.float32).astype(
        jnp.bfloat16
    )
    mir_arrived = exchange(mir_out, half, capacity)

    def expert(rows):
        gate_out = jnp.dot(rows, expert_gate[0], preferred_element_type=jnp.float32)
        up_out = jnp.dot(rows, expert_up[0], preferred_element_type=jnp.float32)
        inner = (jax.nn.silu(gate_out) * up_out).astype(jnp.bfloat16)
        return jnp.dot(inner, expert_down[0], preferred_element_type=jnp.float32).astype(
            jnp.bfloat16
        )

    own_made = expert(own_arrived)
    mir_made = expert(mir_arrived)
    own_made, mir_made = lax.optimization_barrier((own_made, mir_made))
    mir_returned = exchange(mir_made, half, capacity)
    own_returned = exchange(own_made, half, capacity)
    mir_part = scatter_offsets(collect(mir_back, mir_returned), tp_count)
    mir_final = swap(mir_part.astype(jnp.bfloat16), "sp", half)
    own_part = scatter_offsets(collect(own_back, own_returned) + shared_part, tp_count)
    mixed_rows = own_part + mir_final.astype(jnp.float32)
    return (hidden_own.astype(jnp.float32) + mixed_rows).astype(jnp.bfloat16)


def solution(mesh):
    placed = (
        P("sp", "tp"),
        P("sp", "tp"),
        P("sp", "tp"),
        P(),
        P(),
        P("tp"),
        P(),
        P("sp", None),
        P(),
        P("sp", None),
        P("sp", None),
        P(("sp", "tp"), None, None),
        P(("sp", "tp"), None, None),
        P(("sp", "tp"), None, None),
        P(None, "tp"),
        P(None, "tp"),
        P("tp", None),
    )
    return jax.shard_map(
        local, mesh=mesh, in_specs=placed, out_specs=P(("sp", "tp"), None), check_vma=False
    )
```

```python
import jax
import jax.numpy as jnp
from jax import lax
from jax.experimental import pallas as pl
from jax.experimental.pallas import tpu as pltpu
from jax.sharding import PartitionSpec as P

HEAD_SIZE = 64
GRID_W = 64


EPS = 1e-06
THETA = 10000.0


def final_norm(field, gain):
    mean_sq = jnp.mean(field * field, axis=-1, keepdims=True)
    return field * lax.rsqrt(mean_sq + EPS) * gain


def grid_tables(positions, sequence_total):
    grid_rows = sequence_total // GRID_W
    row_pos = (positions // GRID_W - grid_rows // 2).astype(jnp.float32)
    col_pos = (positions % GRID_W - GRID_W // 2).astype(jnp.float32)
    quarter = HEAD_SIZE // 4
    inverse = THETA ** (-jnp.arange(quarter, dtype=jnp.float32) / quarter)
    angles = jnp.concatenate([row_pos[:, None] * inverse, col_pos[:, None] * inverse], axis=1)
    return (jnp.cos(angles), jnp.sin(angles))


def apply_rotary(field, cosine_table, sine_table):
    row_count, head_count = (field.shape[0], field.shape[1])
    quarter = HEAD_SIZE // 4
    pieces = field.reshape(row_count, head_count, 2, 2, quarter)
    front_half = pieces[:, :, :, 0, :].reshape(row_count, head_count, 2 * quarter)
    back_half = pieces[:, :, :, 1, :].reshape(row_count, head_count, 2 * quarter)
    cos_wide = cosine_table[:, None, :]
    sin_wide = sine_table[:, None, :]
    new_front = (front_half * cos_wide - back_half * sin_wide).reshape(
        row_count, head_count, 2, 1, quarter
    )
    new_back = (front_half * sin_wide + back_half * cos_wide).reshape(
        row_count, head_count, 2, 1, quarter
    )
    return jnp.concatenate([new_front, new_back], axis=3).reshape(row_count, head_count, HEAD_SIZE)


def key_block_rows(piece_rows):
    return max((width for width in range(1, 2049) if piece_rows % width == 0))


def swap(field, axis, offset):
    size = lax.axis_size(axis)
    return lax.ppermute(field, axis, [(s, s ^ offset) for s in range(size)])


def by_offset(field, tp_index, tp_count):
    rows = field.shape[0] // tp_count
    return jnp.concatenate(
        [
            lax.dynamic_slice_in_dim(field, jnp.bitwise_xor(tp_index, o) * rows, rows, 0)
            for o in range(tp_count)
        ],
        axis=0,
    )


def gather_offsets(field, tp_count):
    held = {0: field}
    bit = tp_count // 2
    while bit:
        keys = sorted(held)
        sent = jnp.concatenate([held[k] for k in keys], axis=0)
        got = swap(sent, "tp", bit)
        for n, piece in enumerate(jnp.split(got, len(keys), axis=0)):
            held[keys[n] | bit] = piece
        bit //= 2
    return jnp.concatenate([held[k] for k in range(tp_count)], axis=0)


def scatter_step(field, bit, tp_count):
    left = tp_count // bit
    if left < 2:
        return field
    rows = field.shape[0] // left
    pieces = [field[o * rows : (o + 1) * rows] for o in range(left)]
    sent = jnp.concatenate([p.astype(jnp.bfloat16) for p in pieces[1::2]], axis=0)
    got = swap(sent, "tp", bit)
    return jnp.concatenate(pieces[0::2], axis=0) + got.astype(jnp.float32)


def scatter_offsets(field, bit, tp_count):
    while bit < tp_count:
        field = scatter_step(field, bit, tp_count)
        bit *= 2
    return field


def by_block(sp_index, tp_index):
    half = lax.axis_size("sp") // 2
    offsets = jnp.arange(half, dtype=jnp.int32)
    first = (sp_index // half) * half
    targets = first + offsets if half > 8 else jnp.bitwise_xor(sp_index, offsets)
    return targets * lax.axis_size("tp") + tp_index


def slot_map(table, names, sp_index, tp_index):
    topk_count = table.shape[0] // 2
    tokens = table.shape[1]
    experts = names(sp_index, tp_index).astype(jnp.float32)
    match = jnp.zeros((experts.shape[0], tokens), jnp.float32)
    weight = match
    for k in range(topk_count):
        hit = table[k][None, :] == experts[:, None]
        match = match + jnp.where(hit, 1.0, 0.0)
        weight = weight + jnp.where(hit, table[topk_count + k][None, :], 0.0)
    before = jnp.arange(tokens)[:, None] < jnp.arange(tokens)[None, :]
    rank = jnp.dot(
        match.astype(jnp.bfloat16),
        before.astype(jnp.bfloat16),
        preferred_element_type=jnp.float32,
    )
    return match, rank, weight


def filled_slots(match, rank, capacity):
    slots = jnp.arange(capacity, dtype=jnp.int32).astype(jnp.float32)[None, :, None]
    return (rank[:, None, :] == slots) & (match[:, None, :] > 0.5)


def placing(match, rank, capacity):
    filled = filled_slots(match, rank, capacity)
    return jnp.where(filled, 1.0, 0.0).astype(jnp.bfloat16).reshape(-1, match.shape[1])


def weighing(match, rank, weight, capacity):
    filled = filled_slots(match, rank, capacity)
    high = lax.reduce_precision(weight, 8, 7)
    parts = []
    for part in (high, weight - high):
        spread = jnp.where(filled, part[:, None, :], 0.0).astype(jnp.bfloat16)
        parts.append(spread.reshape(-1, match.shape[1]))
    return parts


def collect(back, rows):
    high, low = [
        lax.dot_general(part, rows, (((0,), (0,)), ((), ())), preferred_element_type=jnp.float32)
        for part in back
    ]
    return high + low


def exchange(pieces, half):
    if half > 8:
        size = 2 * half
        groups = [list(range(half)), list(range(half, size))]
        rows = pieces[0]
        return [
            lax.all_to_all(
                rows.reshape(half, rows.shape[0] // half, -1),
                "sp",
                split_axis=0,
                concat_axis=0,
                axis_index_groups=groups,
                tiled=True,
            ).reshape(rows.shape)
        ]
    order = sorted(range(half), key=lambda o: -bin(o).count("1"))
    got = {o: swap(pieces[o], "sp", o) if o else pieces[0] for o in order}
    return [got[o] for o in range(half)]


def cut(rows, half):
    return [rows] if half > 8 else jnp.split(rows, half, axis=0)


def expert_body(*refs):
    count = (len(refs) - 3) // 2
    gate, up, down = refs[count : count + 3]
    rows = jnp.concatenate([r[...] for r in refs[:count]], axis=0)
    gate_out = jnp.dot(rows, gate[...], preferred_element_type=jnp.float32)
    up_out = jnp.dot(rows, up[...], preferred_element_type=jnp.float32)
    inner = (gate_out / (1.0 + jnp.exp(-gate_out)) * up_out).astype(jnp.bfloat16)
    made = jnp.dot(inner, down[...], preferred_element_type=jnp.float32).astype(jnp.bfloat16)
    start = 0
    for out in refs[count + 3 :]:
        out[...] = made[start : start + out.shape[0]]
        start += out.shape[0]


def run_expert(pieces, gate, up, down):
    whole = pl.BlockSpec(memory_space=pltpu.VMEM)
    count = len(pieces)
    return pl.pallas_call(
        expert_body,
        out_shape=[jax.ShapeDtypeStruct(p.shape, p.dtype) for p in pieces],
        in_specs=[whole] * (count + 3),
        out_specs=[whole] * count,
    )(*pieces, gate, up, down)


def gather_blocks(packed, sp_count):
    if sp_count > 8:
        return lax.all_gather(packed, "sp", axis=0, tiled=True)
    order = sorted(range(1, sp_count), reverse=True)
    return jnp.concatenate([swap(packed, "sp", o) for o in order] + [packed], axis=0)


def attention(query_rows, key_values):
    piece_rows = key_values.shape[0]
    block_length = key_block_rows(piece_rows)
    key_blocks = key_values.reshape(piece_rows // block_length, block_length, 2 * HEAD_SIZE)
    score_scale = HEAD_SIZE ** (-0.5)
    rows = query_rows.shape[0]

    def step(carry, key_slab):
        run_max, run_total, run_acc = carry
        scores = (
            lax.dot_general(
                query_rows,
                key_slab[:, :HEAD_SIZE],
                (((1,), (1,)), ((), ())),
                preferred_element_type=jnp.float32,
            )
            * score_scale
        )
        new_max = jnp.maximum(run_max, jnp.max(scores, axis=1))
        factor = jnp.exp(run_max - new_max)
        expo_terms = jnp.exp(scores - new_max[:, None])
        new_total = run_total * factor + jnp.sum(expo_terms, axis=1)
        new_acc = run_acc * factor[:, None] + jnp.dot(
            expo_terms.astype(jnp.bfloat16),
            key_slab[:, HEAD_SIZE:],
            preferred_element_type=jnp.float32,
        )
        return ((new_max, new_total, new_acc), None)

    start = (
        jnp.full((rows,), -1e30, jnp.float32),
        jnp.zeros((rows,), jnp.float32),
        jnp.zeros((rows, HEAD_SIZE), jnp.float32),
    )
    (_, run_total, run_acc), _ = lax.scan(step, start, key_blocks)
    return run_acc / run_total[:, None]


def local(
    queries,
    key_matrix,
    values,
    query_gain,
    key_norm_gain,
    head_gain,
    out_proj,
    residual,
    ffn_gain,
    routes,
    route_weights,
    expert_gate,
    expert_up,
    expert_down,
    shared_gate,
    shared_up,
    shared_down,
):
    tok_count = queries.shape[0]
    head_count = queries.shape[1] // HEAD_SIZE
    sp_count = lax.axis_size("sp")
    tp_count = lax.axis_size("tp")
    tp_index = lax.axis_index("tp")
    sequence_total = tok_count * sp_count
    positions = lax.axis_index("sp") * tok_count + jnp.arange(tok_count, dtype=jnp.int32)
    cosine_table, sine_table = grid_tables(positions, sequence_total)
    rotated_query = apply_rotary(
        final_norm(
            queries.astype(jnp.float32).reshape(tok_count, head_count, HEAD_SIZE), query_gain
        ),
        cosine_table,
        sine_table,
    ).astype(jnp.bfloat16)
    rotated_key = (
        apply_rotary(
            final_norm(
                key_matrix.astype(jnp.float32).reshape(tok_count, 1, HEAD_SIZE), key_norm_gain
            ),
            cosine_table,
            sine_table,
        )
        .reshape(tok_count, HEAD_SIZE)
        .astype(jnp.bfloat16)
    )
    packed = jnp.concatenate([rotated_key, values], axis=1)
    half = sp_count // 2
    sp_index = lax.axis_index("sp")
    part_rows = tok_count // tp_count
    topk_count = routes.shape[1]
    capacity = max(2, 2 * tok_count * topk_count // (sp_count * tp_count))
    table = jnp.concatenate([routes.astype(jnp.float32), route_weights], axis=1)
    own_table = table.T
    mirror_table = by_offset(swap(own_table, "sp", half).T, tp_index, tp_count).T
    own_match, own_rank, own_weight = slot_map(own_table, by_block, sp_index, tp_index)
    mir_match, mir_rank, mir_weight = slot_map(mirror_table, by_block, sp_index, tp_index)
    own_send = placing(own_match, own_rank, capacity)
    mir_send = placing(mir_match, mir_rank, capacity)
    own_back = weighing(
        *[by_offset(m.T, tp_index, tp_count).T for m in (own_match, own_rank, own_weight)],
        capacity,
    )
    mir_back = weighing(mir_match, mir_rank, mir_weight, capacity)

    query_rows = rotated_query.transpose(1, 0, 2).reshape(head_count * tok_count, HEAD_SIZE)
    gathered = gather_blocks(packed, sp_count)
    attended = attention(query_rows, gathered).reshape(head_count, tok_count, HEAD_SIZE)
    attended = attended.transpose(1, 0, 2)
    head_out = final_norm(attended, head_gain.reshape(head_count, HEAD_SIZE)).astype(jnp.bfloat16)
    head_out = head_out.reshape(tok_count, head_count * HEAD_SIZE)
    token_heads = lax.all_gather(head_out, "tp", axis=1, tiled=True)
    hidden = (
        residual.astype(jnp.float32)
        + jnp.dot(token_heads, out_proj, preferred_element_type=jnp.float32)
    ).astype(jnp.bfloat16)
    normed = final_norm(hidden.astype(jnp.float32), ffn_gain).astype(jnp.bfloat16)
    normed_own = lax.dynamic_slice_in_dim(normed, tp_index * part_rows, part_rows, 0)
    hidden_own = lax.dynamic_slice_in_dim(hidden, tp_index * part_rows, part_rows, 0)

    mirror_own = swap(normed_own, "sp", half)
    mirror_rows = gather_offsets(mirror_own, tp_count)
    own_out = jnp.dot(own_send, normed, preferred_element_type=jnp.float32).astype(jnp.bfloat16)
    own_arrived = exchange(cut(own_out, half), half)
    gate_part = jnp.dot(normed, shared_gate, preferred_element_type=jnp.float32)
    up_part = jnp.dot(normed, shared_up, preferred_element_type=jnp.float32)
    shared_inner = (jax.nn.silu(gate_part) * up_part).astype(jnp.bfloat16)
    shared_inner = by_offset(shared_inner, tp_index, tp_count)
    shared_part = jnp.dot(shared_inner, shared_down, preferred_element_type=jnp.float32)

    mir_out = jnp.dot(mir_send, mirror_rows, preferred_element_type=jnp.float32).astype(
        jnp.bfloat16
    )
    mir_arrived = exchange(cut(mir_out, half), half)

    def expert(rows):
        return run_expert(rows, expert_gate[0], expert_up[0], expert_down[0])

    own_made = expert(own_arrived)
    own_made, mir_arrived = lax.optimization_barrier((own_made, mir_arrived))
    mir_made = expert(mir_arrived)
    own_returned = jnp.concatenate(exchange(own_made, half), axis=0)
    mir_returned = jnp.concatenate(exchange(mir_made, half), axis=0)
    mir_pieces = scatter_step(collect(mir_back, mir_returned), 1, tp_count)
    mir_part = scatter_offsets(mir_pieces, 2, tp_count).astype(jnp.bfloat16)
    mir_part, own_back = lax.optimization_barrier((mir_part, own_back))
    mir_final = swap(mir_part, "sp", half)
    own_sum = collect(own_back, own_returned) + shared_part
    own_part = scatter_offsets(scatter_step(own_sum, 1, tp_count), 2, tp_count)
    mixed_rows = own_part + mir_final.astype(jnp.float32)
    return (hidden_own.astype(jnp.float32) + mixed_rows).astype(jnp.bfloat16)


def solution(mesh):
    placed = (
        P("sp", "tp"),
        P("sp", "tp"),
        P("sp", "tp"),
        P(),
        P(),
        P("tp"),
        P(),
        P("sp", None),
        P(),
        P("sp", None),
        P("sp", None),
        P(("sp", "tp"), None, None),
        P(("sp", "tp"), None, None),
        P(("sp", "tp"), None, None),
        P(None, "tp"),
        P(None, "tp"),
        P("tp", None),
    )

    return jax.shard_map(
        local, mesh=mesh, in_specs=placed, out_specs=P(("sp", "tp"), None), check_vma=False
    )
```
